32 devices in a mesh: sp: 4 (over z), dp: 8 (over y, x, core).
Axes of the slice: x: 2, y: 2, z: 4, core: 2. Of those that a mesh axis runs over, the one named last changes fastest.
Arguments:
- cotangent: bfloat16 [8, 512, 2048], P('dp', 'sp'), may hold values from -6 to 6
- unit_pre: bfloat16 [8, 512, 2048], P('dp', None, 'sp'), may hold values from -6 to 6
- gate_pre: bfloat16 [8, 512, 2048], P('dp', None, 'sp'), may hold values from -15 to 15
- out_weight: bfloat16 [2048, 2048], P('dp', 'sp'), may hold values from -0.125 to 0.125
- mix_weight: bfloat16 [8, 128, 128], replicated, may hold values from -0.5 to 0.5
- mix_bias: bfloat16 [8, 128], replicated, may hold values from 0.099609375 to 1.8984375
- norm_gain: bfloat16 [2048], P('sp'), may hold values from 0.099609375 to 1.8984375
- norm_shift: bfloat16 [2048], P('sp'), may hold values from -3 to 3
Outputs:
- unit_grad: bfloat16 [8, 512, 2048], P('dp', None, 'sp')
- gate_grad: bfloat16 [8, 512, 2048], P('dp', None, 'sp')
- out_weight_grad: float32 [2048, 2048], P('dp', 'sp')
- mix_weight_grad: float32 [8, 128, 128], replicated
- mix_bias_grad: float32 [8, 128], replicated
- gain_grad: float32 [2048], P('sp')
- shift_grad: float32 [2048], P('sp')
The draws below stay inside these ranges and needn't reach their ends.
All inputs are finite; a program needn't handle non-finite values.
Results may differ from the reference program's by a relative error of at most 0.015.
Values may be sent and summed in bfloat16 or wider, within the bound.
A program may use at most 64 MiB of HBM per device.

```python
import math
import jax
import jax.numpy as jnp
from jax import lax

D = 2048
GW = 2048
GROUPS = 8
BLK = 128
SEQ = 512
SEQS = 8


def draw_gate_pre(key, part):
    base = jax.random.fold_in(key, 11)
    noise_key, jitter_key = jax.random.split(base, 2)
    position = jnp.arange(GW).astype(jnp.float32) / GW
    jitter = jax.random.uniform(jitter_key, (GW,), jnp.float32, -0.3, 0.3)
    scales = jnp.exp(math.log(0.3) + position * math.log(10.0) + jitter)
    values = jnp.clip(jax.random.normal(noise_key, (SEQS, SEQ, GW), jnp.float32), -3.5, 3.5)
    return (values * scales).astype(jnp.bfloat16)


def block_scale(own_key, shape, shards, least, largest):
    factor_of = 1.0
    for dim, shards_of in shards:
        heights = jax.random.uniform(jax.random.fold_in(jax.random.fold_in(own_key, 6), dim), (shards_of,), jnp.float32, least / len(shards), largest / len(shards))
        factor_of = factor_of * jnp.repeat(jnp.exp(heights), shape[dim] // shards_of).reshape((-1,) + (1,) * (len(shape) - 1 - dim))
    return factor_of


def noise(own_key, extent, width, reach, shards=(), held_as=jnp.bfloat16):
    entries = width * jax.random.normal(own_key, extent, jnp.float32)
    if shards:
        entries = entries * block_scale(own_key, extent, shards, -0.22, 0.18)
    return jnp.clip(entries, -reach, reach).astype(held_as)


def setup_inputs(seed: int = 0) -> dict:
    streams_of = jax.random.split(jax.random.key(seed), 9)
    cotangent = noise(streams_of[0], (SEQS, SEQ, D), 1.0, 6.0, ((0, 8), (1, 4)))
    unit_pre = noise(streams_of[1], (SEQS, SEQ, GW), 1.0, 6.0, ((0, 8), (2, 4)))
    gate_pre = draw_gate_pre(jax.random.fold_in(streams_of[8], 71), 0)
    out_weight = noise(streams_of[3], (D, GW), GW ** -0.5, 0.125, ((0, 8), (1, 4)))
    mix_weight = noise(streams_of[4], (GROUPS, BLK, BLK), BLK ** -0.5, 0.5)
    mix_bias = jnp.clip(1.0 + 0.18 * jax.random.normal(streams_of[5], (GROUPS, BLK), jnp.float32), 0.099609375, 1.8984375).astype(jnp.bfloat16)
    norm_gain = jnp.clip(1.0 + 0.18 * jax.random.normal(streams_of[6], (GW,), jnp.float32), 0.099609375, 1.8984375).astype(jnp.bfloat16)
    norm_shift = noise(streams_of[7], (GW,), 0.5, 3.0, ((0, 4),))
    return {"cotangent": cotangent, "unit_pre": unit_pre, "gate_pre": gate_pre, "out_weight": out_weight, "mix_weight": mix_weight, "mix_bias": mix_bias, "norm_gain": norm_gain, "norm_shift": norm_shift}


epsilon = 1e-05
tanh_coef = math.sqrt(2.0 / math.pi)

def gelu_slope(values):
    inner = tanh_coef * (values + 0.044715 * values * values * values)
    hyper = jnp.tanh(inner)
    return 0.5 * (1.0 + hyper) + 0.5 * values * (1.0 - hyper * hyper) * tanh_coef * (1.0 + 3.0 * 0.044715 * values * values)

def reference(cotangent, unit_pre, gate_pre, out_weight, mix_weight, mix_bias, norm_gain, norm_shift):
    gdim = GW // GROUPS
    blocks = SEQ // BLK
    causal = jnp.arange(BLK)[:, None] >= jnp.arange(BLK)[None, :]
    masked = jnp.where(causal[None], mix_weight.astype(jnp.float32), jnp.float32(0.0))
    bias_full = mix_bias.astype(jnp.float32)
    gain_vec = norm_gain.astype(jnp.float32)
    shift_vec = norm_shift.astype(jnp.float32)

    def one_sequence(totals, inputs):
        dy_seq, unit_seq, gate_seq = inputs
        units = unit_seq.astype(jnp.float32)
        gates = gate_seq.astype(jnp.float32)
        unit_act = jax.nn.gelu(units)
        gate_act = jax.nn.gelu(gates)
        mean_val = lax.optimization_barrier(jnp.mean(gate_act, axis=-1))
        var_val = lax.optimization_barrier(jnp.mean(gate_act * gate_act, axis=-1)) - mean_val * mean_val
        rstd_val = lax.rsqrt(var_val + epsilon)
        centred = (gate_act - mean_val[:, None]) * rstd_val[:, None]
        normed = (centred * gain_vec + shift_vec).astype(jnp.bfloat16)
        normed_blocks = normed.astype(jnp.float32).reshape(blocks, BLK, GROUPS, gdim)
        mixed = jnp.einsum('gts,nsgd->ntgd', masked, normed_blocks) + bias_full.T[None, :, :, None]
        mixed = mixed.reshape(SEQ, GW)
        gated = (unit_act * mixed).astype(jnp.bfloat16)
        head_grad = jnp.dot(dy_seq, out_weight, preferred_element_type=jnp.float32)
        weight_term = lax.dot_general(dy_seq, gated, (((0,), (0,)), ((), ())), preferred_element_type=jnp.float32)
        unit_grad = (head_grad * mixed * gelu_slope(units)).astype(jnp.bfloat16)
        mix_grad = head_grad * unit_act
        mix_round = mix_grad.astype(jnp.bfloat16).astype(jnp.float32).reshape(blocks, BLK, GROUPS, gdim)
        mix_term = jnp.einsum('ntgd,nsgd->gts', mix_round, normed_blocks)
        mix_term = jnp.where(causal[None], mix_term, jnp.float32(0.0))
        bias_term = lax.optimization_barrier(jnp.sum(mix_grad.reshape(blocks, BLK, GROUPS, gdim), axis=(0, 3))).T
        normed_grad = jnp.einsum('gts,ntgd->nsgd', masked, mix_round).reshape(SEQ, GW)
        gain_term = lax.optimization_barrier(jnp.sum(normed_grad * centred, axis=0))
        shift_term = lax.optimization_barrier(jnp.sum(normed_grad, axis=0))
        scaled = normed_grad * gain_vec
        first_m = lax.optimization_barrier(jnp.mean(scaled, axis=-1))
        second_m = lax.optimization_barrier(jnp.mean(scaled * centred, axis=-1))
        gate_grad = (rstd_val[:, None] * (scaled - first_m[:, None] - centred * second_m[:, None]) * gelu_slope(gates)).astype(jnp.bfloat16)
        totals = (totals[0] + weight_term, totals[1] + mix_term, totals[2] + bias_term, totals[3] + gain_term, totals[4] + shift_term)
        return (totals, (unit_grad, gate_grad))
    start_totals = (jnp.zeros((D, GW), jnp.float32), jnp.zeros((GROUPS, BLK, BLK), jnp.float32), jnp.zeros((GROUPS, BLK), jnp.float32), jnp.zeros((GW,), jnp.float32), jnp.zeros((GW,), jnp.float32))
    totals, grads = lax.scan(one_sequence, start_totals, (cotangent, unit_pre, gate_pre))
    token_count = SEQS * SEQ
    norm_scale = 1.0 / math.sqrt(token_count)
    mix_scale = 1.0 / math.sqrt(token_count // BLK * gdim)
    return (grads[0], grads[1], totals[0] * norm_scale, totals[1] * mix_scale, totals[2] * mix_scale, totals[3] * norm_scale, totals[4] * norm_scale)
```

```python
import functools
import math

import jax
import jax.numpy as jnp
from jax import lax
from jax.experimental import pallas as pl
from jax.experimental.pallas import tpu as pltpu
from jax.sharding import PartitionSpec as P

epsilon = 1e-05
tanh_coef = math.sqrt(2.0 / math.pi)
f32 = jnp.float32
bf16 = jnp.bfloat16


def act_and_slope(x):
    square = x * x
    hyper = jnp.tanh(tanh_coef * (x + 0.044715 * square * x))
    half = 0.5 * (1.0 + hyper)
    slope = half + 0.5 * x * (1.0 - hyper * hyper) * tanh_coef * (1.0 + 3.0 * 0.044715 * square)
    return x * half, slope


def xor(value, k):
    bit, out = 0, value
    while (1 << bit) <= k:
        if (k >> bit) & 1:
            out = out + (1 - 2 * ((value // (1 << bit)) % 2)) * (1 << bit)
        bit += 1
    return out


def columns_to_rows(columns, height):
    lane = lax.broadcasted_iota(jnp.int32, (height, 128), 1)
    wide = jnp.zeros((height, 128), f32)
    for i, column in enumerate(columns):
        wide = jnp.where(lane == i, column, wide)
    return jnp.transpose(wide)[0:8]


def rows_to_columns(rows):
    tall = jnp.concatenate([rows, jnp.zeros((120, rows.shape[1]), f32)], axis=0)
    return jnp.transpose(tall)


def kernel(
    n, m, width, group_dim, norm_scale, mix_scale,
    cot, unit, gate, w, mixw, mixb, gain, shift,
    unit_out, gate_out, w_out, mix_out, small_out,
    dyg, wg, cen, gsl, uact, uslope, mixed, normed, gatedt, scaled, acc,
    masked, maskedt, bcol, mixacc, biasacc, vecacc,
    mst, mrv, bst, brv, vst, vrv, vag, mbuf, mrecv, mout,
    part, precv, big, bigrecv,
    ring_s, ring_r, wd_s, wd_r, wf_s, wf_r, m_s, m_r, b_s, b_r, v_s, v_r,
    va_s, va_r, x_s, x_r, xa_s, xa_r, xo_s, xo_r, p_s, p_r, g_s, g_r, loc,
):
    ch = unit.shape[1]
    blk = mixw.shape[1]
    span = min(ch, group_dim)
    gh = ch // span
    dm = w_out.shape[0]
    half = n // 2
    hm = m // 2
    rows = mbuf.shape[1]
    sp = lax.axis_index("sp")
    dp = lax.axis_index("dp")
    core = dp % 2
    pair = dp // 2

    def remote(src, dst, s, r, **where):
        return pltpu.make_async_remote_copy(
            src_ref=src, dst_ref=dst, send_sem=s, recv_sem=r,
            device_id=where, device_id_type=pl.DeviceIdType.MESH,
        )

    def peer_sp(k):
        return (sp + k) % n

    load_c = pltpu.make_async_copy(cot, dyg.at[sp], loc.at[0])
    load_w = pltpu.make_async_copy(w, wg.at[dp], loc.at[1])
    load_c.start()
    load_w.start()
    barrier = pltpu.get_barrier_semaphore()
    for k in range(1, n):
        pl.semaphore_signal(barrier, inc=1, device_id={"sp": peer_sp(k)}, device_id_type=pl.DeviceIdType.MESH)
    for k in range(1, m):
        pl.semaphore_signal(barrier, inc=1, device_id={"dp": xor(dp, k)}, device_id_type=pl.DeviceIdType.MESH)

    def stats(b, carry):
        rs = pl.ds(pl.multiple_of(b * blk, blk), blk)
        value, slope = act_and_slope(gate[rs, :].astype(f32))
        cen[b] = value
        gsl[b] = slope
        mst[b] = columns_to_rows(
            [jnp.sum(value, axis=1, keepdims=True), jnp.sum(value * value, axis=1, keepdims=True)], blk
        )
        return carry

    lax.fori_loop(0, n, stats, 0)
    pl.semaphore_wait(barrier, n + m - 2)
    load_w.wait()

    wd = {
        k: remote(wg.at[dp], wg.at[dp], wd_s.at[k], wd_r.at[k], dp=2 * xor(pair, k) + core)
        for k in range(1, hm)
    }
    for k in reversed(range(1, hm)):
        wd[k].start()
    wf = [
        remote(wg.at[2 * xor(pair, k) + core], wg.at[2 * xor(pair, k) + core],
               wf_s.at[k], wf_r.at[k], dp=xor(dp, 1))
        for k in range(hm)
    ]
    wf[0].start()
    mo = {k: remote(mst, mrv.at[k], m_s.at[k], m_r.at[k], sp=peer_sp(k)) for k in range(1, n)}
    for k in range(1, n):
        mo[k].start()
    load_c.wait()

    def ring(step, direction, full):
        sign = 1 - 2 * direction
        owner = (sp - sign * (step - 1) + 2 * n) % n
        ref = dyg.at[owner]
        if not full:
            cut = blk // 2
            ref = dyg.at[owner, pl.ds(direction * cut, cut)]
        return remote(ref, ref, ring_s.at[direction, step], ring_r.at[direction, step], sp=(sp + sign + n) % n)

    def ring_start(step, full):
        ring(step, 0, full).start()
        ring(step, 1, full).start()

    def ring_recv(step, full):
        ring(step, 0, full).wait_recv()
        ring(step, 1, full).wait_recv()

    ring_start(1, half > 1)

    def units(b, carry):
        rs = pl.ds(pl.multiple_of(b * blk, blk), blk)
        uact[b], uslope[b] = act_and_slope(unit[rs, :].astype(f32))
        return carry

    lax.fori_loop(0, n, units, 0)

    causal = lax.broadcasted_iota(jnp.int32, (blk, blk), 0) >= lax.broadcasted_iota(jnp.int32, (blk, blk), 1)
    lane = lax.broadcasted_iota(jnp.int32, (blk, 128), 1)
    bias_t = rows_to_columns(mixb[...].astype(f32))
    start = sp * ch // group_dim
    for g in range(gh):
        one = jnp.where(causal, mixw[start + g].astype(f32), 0.0)
        masked[g] = one.astype(bf16)
        maskedt[g] = jnp.transpose(one).astype(bf16)
        bcol[g] = jnp.broadcast_to(
            jnp.sum(jnp.where(lane == start + g, bias_t, 0.0), axis=1, keepdims=True), (blk, 128)
        )
    gain_row = gain[...].astype(f32)
    shift_row = shift[...].astype(f32)
    for k in range(1, n):
        mo[k].wait_recv()

    def forward(b, carry):
        total = mst[b]
        for k in range(1, n):
            total = total + mrv[k, b]
        cols = rows_to_columns(total)
        mean = cols[:, 0:1] / width
        var = cols[:, 1:2] / width - mean * mean
        rstd = lax.rsqrt(var + epsilon)
        centred = (cen[b] - mean) * rstd
        cen[b] = centred
        gsl[b] = gsl[b] * rstd
        nb = (centred * gain_row + shift_row).astype(bf16)
        normed[b] = nb
        for g in range(gh):
            cs = slice(g * span, (g + 1) * span)
            mixg = jnp.dot(masked[g], nb[:, cs], preferred_element_type=f32) + bcol[g][:, 0:1]
            mixed[b, :, cs] = mixg
            gatedt[b, cs, :] = jnp.transpose(uact[b, :, cs] * mixg).astype(bf16)
        return carry

    lax.fori_loop(0, n, forward, 0)
    mixacc[...] = jnp.zeros_like(mixacc)
    biasacc[...] = jnp.zeros_like(biasacc)
    vecacc[...] = jnp.zeros_like(vecacc)

    ring_recv(1, half > 1)
    if half > 1:
        ring_start(2, half > 2)
    for k in reversed(range(1, hm)):
        wd[k].wait_recv()
        wf[k].start()
    for k in range(hm):
        wf[k].wait_recv()

    def block(o):
        rs = pl.ds(pl.multiple_of(o * blk, blk), blk)
        whole = wg[...].reshape(m * dm, ch)
        head = jnp.dot(dyg[o], whole, preferred_element_type=f32)
        unit_out[rs, :] = (head * mixed[o] * uslope[o]).astype(bf16)
        grad = head * uact[o]
        biasacc[...] += grad
        rounded = grad.astype(bf16)
        first = jnp.zeros((blk, 1), f32)
        second = jnp.zeros((blk, 1), f32)
        for g in range(gh):
            cs = slice(g * span, (g + 1) * span)
            mixacc[g] += lax.dot_general(
                rounded[:, cs], normed[o, :, cs], (((1,), (1,)), ((), ())), preferred_element_type=f32
            )
            ng = jnp.dot(maskedt[g], rounded[:, cs], preferred_element_type=f32)
            centred = cen[o, :, cs]
            vecacc[0:1, cs] += jnp.sum(ng * centred, axis=0, keepdims=True)
            vecacc[1:2, cs] += jnp.sum(ng, axis=0, keepdims=True)
            sc = ng * gain_row[:, cs]
            scaled[o, :, cs] = sc
            first = first + jnp.sum(sc, axis=1, keepdims=True)
            second = second + jnp.sum(sc * centred, axis=1, keepdims=True)
        bst[o] = columns_to_rows([first, second], blk)

    def weight(o, k):
        return jnp.dot(gatedt[o], dyg[o, :, k * dm:(k + 1) * dm], preferred_element_type=f32)

    def weights(o):
        for k in range(m):
            acc[k] += weight(o, k)

    block(sp)
    for k in range(m):
        acc[k] = weight(sp, k)

    def middle(step):
        def one(side, carry):
            o = (sp + (2 * side - 1) * step + n) % n
            block(o)
            weights(o)
            return carry

        lax.fori_loop(0, 2, one, 0)

    for step in range(1, half):
        if step > 1:
            ring_recv(step, True)
            ring_start(step + 1, step + 1 < half)
        middle(step)
    if half > 1:
        ring_recv(half, False)
    last = (sp + half) % n
    block(last)

    for g in range(gh):
        one = jnp.where(causal, mixacc[g], 0.0).astype(bf16)
        per = blk // rows
        for i in range(per):
            mbuf[g * per + i] = one[i * rows:(i + 1) * rows]
    bias_rows = columns_to_rows(
        [jnp.sum(biasacc[:, g * span:(g + 1) * span], axis=1, keepdims=True) for g in range(gh)], blk
    )
    vst[0:2, :] = vecacc[0:2, :]
    vst[2:2 + gh, 0:blk] = bias_rows[0:gh]
    xo = {k: remote(mbuf.at[xor(dp, k)], mrecv.at[k], x_s.at[k], x_r.at[k], dp=xor(dp, k)) for k in range(1, m)}
    vo = {k: remote(vst, vrv.at[k], v_s.at[k], v_r.at[k], dp=xor(dp, k)) for k in range(1, m)}
    bo = {k: remote(bst, brv.at[k], b_s.at[k], b_r.at[k], sp=peer_sp(k)) for k in range(1, n)}
    for k in reversed(range(1, m)):
        xo[k].start()
    for k in reversed(range(1, m)):
        vo[k].start()
    for k in range(1, n):
        bo[k].start()

    for k in range(m):
        acc[k] += weight(last, k)
    po = {}
    for k in reversed(range(hm)):
        other = 2 * xor(pair, k) + 1 - core
        part[k] = acc[other].astype(bf16)
        po[k] = remote(part.at[k], precv.at[k], p_s.at[k], p_r.at[k], dp=xor(dp, 1))
        po[k].start()

    for k in range(1, m):
        xo[k].wait_recv()
    total = mbuf[dp].astype(f32)
    for k in range(1, m):
        total = total + mrecv[k].astype(f32)
    mout[sp, dp] = total.astype(bf16)
    xa = {
        k: remote(mout.at[sp, dp], mout.at[sp, dp], xa_s.at[k], xa_r.at[k], dp=xor(dp, k)) for k in range(1, m)
    }
    for k in reversed(range(1, m)):
        xa[k].start()

    go = {}
    for k in reversed(range(1, hm)):
        po[k].wait_recv()
        big[k] = (acc[2 * xor(pair, k) + core] + precv[k].astype(f32)).astype(bf16)
        go[k] = remote(big.at[k], bigrecv.at[k], g_s.at[k], g_r.at[k], dp=2 * xor(pair, k) + core)
        go[k].start()
    po[0].wait_recv()

    for k in range(1, m):
        vo[k].wait_recv()
    vec = vst[...]
    for k in range(1, m):
        vec = vec + vrv[k]
    vag[sp] = vec
    va = {k: remote(vag.at[sp], vag.at[sp], va_s.at[k], va_r.at[k], sp=peer_sp(k)) for k in range(1, n)}
    for k in range(1, n):
        va[k].start()
    for k in range(1, m):
        xa[k].wait_recv()
    xs = {k: remote(mout.at[sp], mout.at[sp], xo_s.at[k], xo_r.at[k], sp=peer_sp(k)) for k in range(1, n)}
    for k in range(1, n):
        xs[k].start()

    for k in range(1, n):
        bo[k].wait_recv()

    def finish(b, carry):
        rs = pl.ds(pl.multiple_of(b * blk, blk), blk)
        total = bst[b]
        for k in range(1, n):
            total = total + brv[k, b]
        cols = rows_to_columns(total)
        gate_out[rs, :] = (
            gsl[b] * (scaled[b] - cols[:, 0:1] / width - cen[b] * (cols[:, 1:2] / width))
        ).astype(bf16)
        return carry

    lax.fori_loop(0, n, finish, 0)
    for k in range(1, n):
        va[k].wait_recv()
    small_out[...] = vag[...]
    for k in range(1, n):
        xs[k].wait_recv()
    mix_out[...] = mout[...].astype(f32) * mix_scale

    own = acc[dp] + precv[0].astype(f32)
    for k in range(1, hm):
        go[k].wait_recv()
        own = own + bigrecv[k].astype(f32)
    w_out[...] = jnp.transpose(own * norm_scale)

    for step in range(1, half + 1):
        ring(step, 0, step < half).wait_send()
        ring(step, 1, step < half).wait_send()
    sent = list(wd.values()) + wf + list(po.values())
    for group in (mo, xo, vo, bo, xa, go, va, xs):
        sent += list(group.values())
    for copy in sent:
        copy.wait_send()


def local(cotangent, unit_pre, gate_pre, out_weight, mix_weight, mix_bias, norm_gain, norm_shift):
    n, m = lax.axis_size("sp"), lax.axis_size("dp")
    groups, blk = mix_bias.shape
    seq, ch = unit_pre.shape[1:]
    width = ch * n
    dm, d = out_weight.shape[0], cotangent.shape[2]
    group_dim = width // groups
    span = min(ch, group_dim)
    gh = ch // span
    assert cotangent.shape[1] == blk and n % 2 == 0 and m & (m - 1) == 0
    rows = gh * blk // m
    hm = m // 2
    tokens = m * seq
    norm_scale = 1.0 / math.sqrt(tokens)
    mix_scale = 1.0 / math.sqrt(tokens // blk * group_dim)
    vm = pl.BlockSpec(memory_space=pltpu.VMEM)
    hbm = pl.BlockSpec(memory_space=pl.ANY)
    V = pltpu.VMEM
    dma = pltpu.SemaphoreType.DMA
    scratch = [
        V((n, blk, d), bf16), V((m, dm, ch), bf16),
        V((n, blk, ch), f32), V((n, blk, ch), f32), V((n, blk, ch), f32), V((n, blk, ch), f32),
        V((n, blk, ch), f32), V((n, blk, ch), bf16), V((n, ch, blk), bf16), V((n, blk, ch), f32),
        V((m, ch, dm), f32),
        V((gh, blk, blk), bf16), V((gh, blk, blk), bf16), V((gh, blk, 128), f32),
        V((gh, blk, blk), f32), V((blk, ch), f32), V((8, ch), f32),
        V((n, 8, blk), f32), V((n, n, 8, blk), f32), V((n, 8, blk), f32), V((n, n, 8, blk), f32),
        V((8, ch), f32), V((m, 8, ch), f32), V((n, 8, ch), f32),
        V((m, rows, blk), bf16), V((m, rows, blk), bf16), V((n, m, rows, blk), bf16),
        V((hm, ch, dm), bf16), V((hm, ch, dm), bf16), V((hm, ch, dm), bf16), V((hm, ch, dm), bf16),
        dma((2, n)), dma((2, n)),
        dma((hm,)), dma((hm,)), dma((hm,)), dma((hm,)),
        dma((n,)), dma((n,)), dma((n,)), dma((n,)), dma((m,)), dma((m,)),
        dma((n,)), dma((n,)), dma((m,)), dma((m,)), dma((m,)), dma((m,)), dma((n,)), dma((n,)),
        dma((hm,)), dma((hm,)), dma((hm,)), dma((hm,)), dma((2,)),
    ]
    unit_grad, gate_grad, w_grad, mix, small = pl.pallas_call(
        functools.partial(kernel, n, m, width, group_dim, norm_scale, mix_scale),
        out_shape=(
            jax.ShapeDtypeStruct((seq, ch), bf16),
            jax.ShapeDtypeStruct((seq, ch), bf16),
            jax.ShapeDtypeStruct((dm, ch), f32),
            jax.ShapeDtypeStruct((n, m, rows, blk), f32),
            jax.ShapeDtypeStruct((n, 8, ch), f32),
        ),
        in_specs=[hbm, vm, vm, hbm, vm, vm, vm, vm],
        out_specs=(vm,) * 5,
        scratch_shapes=scratch,
        compiler_params=pltpu.CompilerParams(
            collective_id=0, has_side_effects=True, vmem_limit_bytes=60 * 1024 * 1024
        ),
    )(
        cotangent[0], unit_pre[0], gate_pre[0], out_weight, mix_weight, mix_bias,
        norm_gain[None], norm_shift[None],
    )
    share = group_dim // span
    mix = jnp.sum(mix.reshape(groups, share, blk, blk), axis=1)
    bias = jnp.sum(small[:, 2:2 + gh, :blk].reshape(groups, share, blk), axis=1) * mix_scale
    mine = lax.dynamic_index_in_dim(small, lax.axis_index("sp"), 0, keepdims=False)
    return (
        unit_grad[None], gate_grad[None], w_grad, mix, bias, mine[0] * norm_scale, mine[1] * norm_scale,
    )


def solution(mesh):
    in_specs = (
        P("dp", "sp", None),
        P("dp", None, "sp"),
        P("dp", None, "sp"),
        P("dp", "sp"),
        P(),
        P(),
        P("sp"),
        P("sp"),
    )
    out_specs = (
        P("dp", None, "sp"),
        P("dp", None, "sp"),
        P("dp", "sp"),
        P(),
        P(),
        P("sp"),
        P("sp"),
    )
    return jax.shard_map(local, mesh=mesh, in_specs=in_specs, out_specs=out_specs, check_vma=False)
```

```python
import functools
import math

import jax
import jax.numpy as jnp
from jax import lax
from jax.experimental import pallas as pl
from jax.experimental.pallas import tpu as pltpu
from jax.sharding import PartitionSpec as P

epsilon = 1e-05
tanh_coef = math.sqrt(2.0 / math.pi)
f32 = jnp.float32
bf16 = jnp.bfloat16


def act_and_slope(x):
    square = x * x
    hyper = jnp.tanh(tanh_coef * (x + 0.044715 * square * x))
    half = 0.5 * (1.0 + hyper)
    slope = half + 0.5 * x * (1.0 - hyper * hyper) * tanh_coef * (1.0 + 3.0 * 0.044715 * square)
    return x * half, slope


def xor(value, k):
    bit, out = 0, value
    while (1 << bit) <= k:
        if (k >> bit) & 1:
            out = out + (1 - 2 * ((value // (1 << bit)) % 2)) * (1 << bit)
        bit += 1
    return out


def columns_to_rows(columns, height):
    lane = lax.broadcasted_iota(jnp.int32, (height, 128), 1)
    wide = jnp.zeros((height, 128), f32)
    for i, column in enumerate(columns):
        wide = jnp.where(lane == i, column, wide)
    return jnp.transpose(wide)[0:8]


def rows_to_columns(rows):
    tall = jnp.concatenate([rows, jnp.zeros((120, rows.shape[1]), f32)], axis=0)
    return jnp.transpose(tall)


def kernel(
    n, m, width, group_dim, norm_scale, mix_scale,
    cot, unit, gate, w, mixw, mixb, gain, shift,
    unit_out, gate_out, w_out, mix_out, small_out,
    dyg, wg, cen, gsl, uact, uslope, mixed, normed, gatedt, scaled, acc,
    masked, maskedt, bcol, mixacc, biasacc, vecacc,
    mst, mrv, bst, brv, vst, vrv, vag, mbuf, mrecv, mout,
    part, precv, big, bigrecv,
    ring_s, ring_r, wd_s, wd_r, wf_s, wf_r, m_s, m_r, b_s, b_r, v_s, v_r,
    va_s, va_r, x_s, x_r, xa_s, xa_r, xo_s, xo_r, xf_s, xf_r, p_s, p_r, g_s, g_r, loc,
):
    ch = unit.shape[1]
    blk = mixw.shape[1]
    span = min(ch, group_dim)
    gh = ch // span
    dm = w_out.shape[0]
    half = n // 2
    hm = m // 2
    rows = mbuf.shape[1]
    sp = lax.axis_index("sp")
    dp = lax.axis_index("dp")
    core = dp % 2
    pair = dp // 2

    def remote(src, dst, s, r, **where):
        return pltpu.make_async_remote_copy(
            src_ref=src, dst_ref=dst, send_sem=s, recv_sem=r,
            device_id=where, device_id_type=pl.DeviceIdType.MESH,
        )

    def peer_sp(k):
        return (sp + k) % n

    load_c = pltpu.make_async_copy(cot, dyg.at[sp], loc.at[0])
    load_w = pltpu.make_async_copy(w, wg.at[dp], loc.at[1])
    load_c.start()
    load_w.start()
    barrier = pltpu.get_barrier_semaphore()
    for k in range(1, n):
        pl.semaphore_signal(barrier, inc=1, device_id={"sp": peer_sp(k)}, device_id_type=pl.DeviceIdType.MESH)
    for k in range(1, m):
        pl.semaphore_signal(barrier, inc=1, device_id={"dp": xor(dp, k)}, device_id_type=pl.DeviceIdType.MESH)

    def stats(b, carry):
        rs = pl.ds(pl.multiple_of(b * blk, blk), blk)
        value, slope = act_and_slope(gate[rs, :].astype(f32))
        cen[b] = value
        gsl[b] = slope
        mst[b] = columns_to_rows(
            [jnp.sum(value, axis=1, keepdims=True), jnp.sum(value * value, axis=1, keepdims=True)], blk
        )
        return carry

    lax.fori_loop(0, n, stats, 0)
    pl.semaphore_wait(barrier, n + m - 2)
    load_w.wait()

    wd = {
        k: remote(wg.at[dp], wg.at[dp], wd_s.at[k], wd_r.at[k], dp=2 * xor(pair, k) + core)
        for k in range(1, hm)
    }
    for k in reversed(range(1, hm)):
        wd[k].start()
    wf = [
        remote(wg.at[2 * xor(pair, k) + core], wg.at[2 * xor(pair, k) + core],
               wf_s.at[k], wf_r.at[k], dp=xor(dp, 1))
        for k in range(hm)
    ]
    wf[0].start()
    mo = {k: remote(mst, mrv.at[k], m_s.at[k], m_r.at[k], sp=peer_sp(k)) for k in range(1, n)}
    for k in range(1, n):
        mo[k].start()
    load_c.wait()

    def ring(step, direction, piece):
        sign = 1 - 2 * direction
        owner = (sp - sign * (step - 1) + 2 * n) % n
        cut = blk // 2
        ref = dyg.at[owner, pl.ds((direction + piece) % 2 * cut, cut)]
        lane = 2 * direction + piece
        return remote(ref, ref, ring_s.at[lane, step], ring_r.at[lane, step], sp=(sp + sign + n) % n)

    def ring_start(step, piece):
        ring(step, 0, piece).start()
        ring(step, 1, piece).start()

    def ring_recv(step, piece):
        ring(step, 0, piece).wait_recv()
        ring(step, 1, piece).wait_recv()

    def ring_pass(step, piece):
        ring_recv(step, piece)
        if piece == 0 or step + 1 < half:
            ring_start(step + 1, piece)

    ring_start(1, 0)
    if half > 1:
        ring_start(1, 1)

    def units(b, carry):
        rs = pl.ds(pl.multiple_of(b * blk, blk), blk)
        uact[b], uslope[b] = act_and_slope(unit[rs, :].astype(f32))
        return carry

    lax.fori_loop(0, n, units, 0)

    causal = lax.broadcasted_iota(jnp.int32, (blk, blk), 0) >= lax.broadcasted_iota(jnp.int32, (blk, blk), 1)
    lane = lax.broadcasted_iota(jnp.int32, (blk, 128), 1)
    bias_t = rows_to_columns(mixb[...].astype(f32))
    start = sp * ch // group_dim
    for g in range(gh):
        one = jnp.where(causal, mixw[start + g].astype(f32), 0.0)
        masked[g] = one.astype(bf16)
        maskedt[g] = jnp.transpose(one).astype(bf16)
        bcol[g] = jnp.broadcast_to(
            jnp.sum(jnp.where(lane == start + g, bias_t, 0.0), axis=1, keepdims=True), (blk, 128)
        )
    gain_row = gain[...].astype(f32)
    shift_row = shift[...].astype(f32)
    for k in range(1, n):
        mo[k].wait_recv()

    def forward(b, carry):
        total = mst[b]
        for k in range(1, n):
            total = total + mrv[k, b]
        cols = rows_to_columns(total)
        mean = cols[:, 0:1] / width
        var = cols[:, 1:2] / width - mean * mean
        rstd = lax.rsqrt(var + epsilon)
        centred = (cen[b] - mean) * rstd
        cen[b] = centred
        gsl[b] = gsl[b] * rstd
        nb = (centred * gain_row + shift_row).astype(bf16)
        normed[b] = nb
        for g in range(gh):
            cs = slice(g * span, (g + 1) * span)
            mixg = jnp.dot(masked[g], nb[:, cs], preferred_element_type=f32) + bcol[g][:, 0:1]
            mixed[b, :, cs] = mixg
            gatedt[b, cs, :] = jnp.transpose(uact[b, :, cs] * mixg).astype(bf16)
        return carry

    lax.fori_loop(0, n, forward, 0)
    if half > 1:
        ring_pass(1, 0)
    mixacc[...] = jnp.zeros_like(mixacc)
    biasacc[...] = jnp.zeros_like(biasacc)
    vecacc[...] = jnp.zeros_like(vecacc)

    for k in reversed(range(1, hm)):
        wd[k].wait_recv()
        wf[k].start()
    for k in range(hm):
        wf[k].wait_recv()

    def block(o):
        rs = pl.ds(pl.multiple_of(o * blk, blk), blk)
        whole = wg[...].reshape(m * dm, ch)
        head = jnp.dot(dyg[o], whole, preferred_element_type=f32)
        unit_out[rs, :] = (head * mixed[o] * uslope[o]).astype(bf16)
        grad = head * uact[o]
        biasacc[...] += grad
        rounded = grad.astype(bf16)
        first = jnp.zeros((blk, 1), f32)
        second = jnp.zeros((blk, 1), f32)
        for g in range(gh):
            cs = slice(g * span, (g + 1) * span)
            mixacc[g] += lax.dot_general(
                rounded[:, cs], normed[o, :, cs], (((1,), (1,)), ((), ())), preferred_element_type=f32
            )
            ng = jnp.dot(maskedt[g], rounded[:, cs], preferred_element_type=f32)
            centred = cen[o, :, cs]
            vecacc[0:1, cs] += jnp.sum(ng * centred, axis=0, keepdims=True)
            vecacc[1:2, cs] += jnp.sum(ng, axis=0, keepdims=True)
            sc = ng * gain_row[:, cs]
            scaled[o, :, cs] = sc
            first = first + jnp.sum(sc, axis=1, keepdims=True)
            second = second + jnp.sum(sc * centred, axis=1, keepdims=True)
        bst[o] = columns_to_rows([first, second], blk)

    def weight(o, k):
        return jnp.dot(gatedt[o], dyg[o, :, k * dm:(k + 1) * dm], preferred_element_type=f32)

    def weights(o):
        for k in range(m):
            acc[k] += weight(o, k)

    block(sp)
    for k in range(m):
        acc[k] = weight(sp, k)

    def middle(step):
        def one(side, carry):
            o = (sp + (2 * side - 1) * step + n) % n
            block(o)
            weights(o)
            return carry

        lax.fori_loop(0, 2, one, 0)

    for step in range(1, half):
        if step > 1:
            ring_pass(step, 0)
        ring_pass(step, 1)
        middle(step)
    ring_recv(half, 0)
    last = (sp + half) % n
    block(last)

    for g in range(gh):
        one = jnp.where(causal, mixacc[g], 0.0).astype(bf16)
        per = blk // rows
        for i in range(per):
            mbuf[g * per + i] = one[i * rows:(i + 1) * rows]
    bias_rows = columns_to_rows(
        [jnp.sum(biasacc[:, g * span:(g + 1) * span], axis=1, keepdims=True) for g in range(gh)], blk
    )
    vst[0:2, :] = vecacc[0:2, :]
    vst[2:2 + gh, 0:blk] = bias_rows[0:gh]
    xo = {k: remote(mbuf.at[xor(dp, k)], mrecv.at[k], x_s.at[k], x_r.at[k], dp=xor(dp, k)) for k in range(1, m)}
    vo = {k: remote(vst, vrv.at[k], v_s.at[k], v_r.at[k], dp=xor(dp, k)) for k in range(1, m)}
    bo = {k: remote(bst, brv.at[k], b_s.at[k], b_r.at[k], sp=peer_sp(k)) for k in range(1, n)}
    for k in reversed(range(1, m)):
        xo[k].start()
    for k in reversed(range(1, m)):
        vo[k].start()
    for k in range(1, n):
        bo[k].start()

    for k in range(m):
        acc[k] += weight(last, k)
    po = {}
    for k in reversed(range(hm)):
        other = 2 * xor(pair, k) + 1 - core
        part[k] = acc[other].astype(bf16)
        po[k] = remote(part.at[k], precv.at[k], p_s.at[k], p_r.at[k], dp=xor(dp, 1))
        po[k].start()

    for k in range(1, m):
        xo[k].wait_recv()
    total = mbuf[dp].astype(f32)
    for k in range(1, m):
        total = total + mrecv[k].astype(f32)
    mout[sp, dp] = total.astype(bf16)
    xa = {
        k: remote(mout.at[sp, dp], mout.at[sp, dp], xa_s.at[k], xa_r.at[k], dp=xor(dp, k)) for k in range(1, m)
    }
    for k in reversed(range(1, m)):
        xa[k].start()

    go = {}
    for k in reversed(range(1, hm)):
        po[k].wait_recv()
        big[k] = (acc[2 * xor(pair, k) + core] + precv[k].astype(f32)).astype(bf16)
        go[k] = remote(big.at[k], bigrecv.at[k], g_s.at[k], g_r.at[k], dp=2 * xor(pair, k) + core)
        go[k].start()
    po[0].wait_recv()

    for k in range(1, m):
        vo[k].wait_recv()
    vec = vst[...]
    for k in range(1, m):
        vec = vec + vrv[k]
    vag[sp] = vec
    va = {k: remote(vag.at[sp], vag.at[sp], va_s.at[k], va_r.at[k], sp=peer_sp(k)) for k in range(1, n)}
    for k in range(1, n):
        va[k].start()
    for k in range(1, m):
        xa[k].wait_recv()
    share = pl.ds(core * hm, hm)
    xs = {
        k: remote(mout.at[sp, share], mout.at[sp, share], xo_s.at[k], xo_r.at[k], sp=peer_sp(k))
        for k in range(1, n)
    }
    xf = {
        k: remote(mout.at[(sp - k + n) % n, share], mout.at[(sp - k + n) % n, share],
                  xf_s.at[k], xf_r.at[k], dp=xor(dp, 1))
        for k in range(1, n)
    }
    for k in range(1, n):
        xs[k].start()

    for k in range(1, n):
        bo[k].wait_recv()

    def finish(b, carry):
        rs = pl.ds(pl.multiple_of(b * blk, blk), blk)
        total = bst[b]
        for k in range(1, n):
            total = total + brv[k, b]
        cols = rows_to_columns(total)
        gate_out[rs, :] = (
            gsl[b] * (scaled[b] - cols[:, 0:1] / width - cen[b] * (cols[:, 1:2] / width))
        ).astype(bf16)
        return carry

    lax.fori_loop(0, n, finish, 0)
    for k in range(1, n):
        va[k].wait_recv()
    small_out[...] = vag[...]
    for k in range(1, n):
        xs[k].wait_recv()
        xf[k].start()
    for k in range(1, n):
        xf[k].wait_recv()
    mix_out[...] = mout[...].astype(f32) * mix_scale

    own = acc[dp] + precv[0].astype(f32)
    for k in range(1, hm):
        go[k].wait_recv()
        own = own + bigrecv[k].astype(f32)
    w_out[...] = jnp.transpose(own * norm_scale)

    for step in range(1, half + 1):
        for piece in range(2 if step < half else 1):
            ring(step, 0, piece).wait_send()
            ring(step, 1, piece).wait_send()
    sent = list(wd.values()) + wf + list(po.values())
    for group in (mo, xo, vo, bo, xa, go, va, xs, xf):
        sent += list(group.values())
    for copy in sent:
        copy.wait_send()


def finish_kernel(
    share, mix_scale, norm_scale, unit_in, gate_in, w_in, mix_in, small_in,
    unit_out, gate_out, w_out, mix_out, bias_out, gain_out, shift_out, sems,
):
    copies = [
        pltpu.make_async_copy(src, dst, sems.at[i])
        for i, (src, dst) in enumerate(
            ((unit_in, unit_out.at[0]), (gate_in, gate_out.at[0]), (w_in, w_out), (mix_in, mix_out))
        )
    ]
    for copy in copies:
        copy.start()
    groups, blk = bias_out.shape
    n = small_in.shape[0]
    gh = groups * share // n
    for g in range(groups):
        total = 0.0
        for part in range(g * share, (g + 1) * share):
            row = 2 + part % gh
            total = total + small_in[part // gh, row:row + 1, 0:blk]
        bias_out[g:g + 1, :] = total * mix_scale
    mine = small_in[lax.axis_index("sp")] * norm_scale
    gain_out[...] = mine[0:1]
    shift_out[...] = mine[1:2]
    for copy in copies:
        copy.wait()


def local(cotangent, unit_pre, gate_pre, out_weight, mix_weight, mix_bias, norm_gain, norm_shift):
    n, m = lax.axis_size("sp"), lax.axis_size("dp")
    groups, blk = mix_bias.shape
    seq, ch = unit_pre.shape[1:]
    width = ch * n
    dm, d = out_weight.shape[0], cotangent.shape[2]
    group_dim = width // groups
    span = min(ch, group_dim)
    gh = ch // span
    assert cotangent.shape[1] == blk and n % 2 == 0 and m & (m - 1) == 0
    rows = gh * blk // m
    hm = m // 2
    tokens = m * seq
    norm_scale = 1.0 / math.sqrt(tokens)
    mix_scale = 1.0 / math.sqrt(tokens // blk * group_dim)
    vm = pl.BlockSpec(memory_space=pltpu.VMEM)
    hbm = pl.BlockSpec(memory_space=pl.ANY)
    V = pltpu.VMEM
    dma = pltpu.SemaphoreType.DMA
    scratch = [
        V((n, blk, d), bf16), V((m, dm, ch), bf16),
        V((n, blk, ch), f32), V((n, blk, ch), f32), V((n, blk, ch), f32), V((n, blk, ch), f32),
        V((n, blk, ch), f32), V((n, blk, ch), bf16), V((n, ch, blk), bf16), V((n, blk, ch), f32),
        V((m, ch, dm), f32),
        V((gh, blk, blk), bf16), V((gh, blk, blk), bf16), V((gh, blk, 128), f32),
        V((gh, blk, blk), f32), V((blk, ch), f32), V((8, ch), f32),
        V((n, 8, blk), f32), V((n, n, 8, blk), f32), V((n, 8, blk), f32), V((n, n, 8, blk), f32),
        V((8, ch), f32), V((m, 8, ch), f32), V((n, 8, ch), f32),
        V((m, rows, blk), bf16), V((m, rows, blk), bf16), V((n, m, rows, blk), bf16),
        V((hm, ch, dm), bf16), V((hm, ch, dm), bf16), V((hm, ch, dm), bf16), V((hm, ch, dm), bf16),
        dma((4, n)), dma((4, n)),
        dma((hm,)), dma((hm,)), dma((hm,)), dma((hm,)),
        dma((n,)), dma((n,)), dma((n,)), dma((n,)), dma((m,)), dma((m,)),
        dma((n,)), dma((n,)), dma((m,)), dma((m,)), dma((m,)), dma((m,)), dma((n,)), dma((n,)),
        dma((n,)), dma((n,)),
        dma((hm,)), dma((hm,)), dma((hm,)), dma((hm,)), dma((2,)),
    ]
    unit_grad, gate_grad, w_grad, mix, small = pl.pallas_call(
        functools.partial(kernel, n, m, width, group_dim, norm_scale, mix_scale),
        out_shape=(
            jax.ShapeDtypeStruct((seq, ch), bf16),
            jax.ShapeDtypeStruct((seq, ch), bf16),
            jax.ShapeDtypeStruct((dm, ch), f32),
            jax.ShapeDtypeStruct((n, m, rows, blk), f32),
            jax.ShapeDtypeStruct((n, 8, ch), f32),
        ),
        in_specs=[hbm, vm, vm, hbm, vm, vm, vm, vm],
        out_specs=(vm,) * 5,
        scratch_shapes=scratch,
        compiler_params=pltpu.CompilerParams(
            collective_id=0, has_side_effects=True, vmem_limit_bytes=60 * 1024 * 1024
        ),
    )(
        cotangent[0], unit_pre[0], gate_pre[0], out_weight, mix_weight, mix_bias,
        norm_gain[None], norm_shift[None],
    )
    share = group_dim // span
    unit_grad, gate_grad, w_grad, mix, bias, gain_grad, shift_grad = pl.pallas_call(
        functools.partial(finish_kernel, share, mix_scale, norm_scale),
        out_shape=(
            jax.ShapeDtypeStruct((1, seq, ch), bf16),
            jax.ShapeDtypeStruct((1, seq, ch), bf16),
            jax.ShapeDtypeStruct((dm, ch), f32),
            jax.ShapeDtypeStruct((n, m, rows, blk), f32),
            jax.ShapeDtypeStruct((groups, blk), f32),
            jax.ShapeDtypeStruct((1, ch), f32),
            jax.ShapeDtypeStruct((1, ch), f32),
        ),
        in_specs=[vm] * 5,
        out_specs=(hbm,) * 4 + (vm,) * 3,
        scratch_shapes=[dma((4,))],
    )(unit_grad, gate_grad, w_grad, mix, small)
    if share == 1:
        mix = mix.reshape(groups, blk, blk)
    else:
        mix = jnp.sum(mix.reshape(groups, share, blk, blk), axis=1)
    return unit_grad, gate_grad, w_grad, mix, bias, gain_grad[0], shift_grad[0]


def solution(mesh):
    in_specs = (
        P("dp", "sp", None),
        P("dp", None, "sp"),
        P("dp", None, "sp"),
        P("dp", "sp"),
        P(),
        P(),
        P("sp"),
        P("sp"),
    )
    out_specs = (
        P("dp", None, "sp"),
        P("dp", None, "sp"),
        P("dp", "sp"),
        P(),
        P(),
        P("sp"),
        P("sp"),
    )
    return jax.shard_map(local, mesh=mesh, in_specs=in_specs, out_specs=out_specs, check_vma=False)
```
